32 devices in a mesh: sp: 16 (over z, y, x), tp: 2 (over core).
Axes of the slice: x: 2, y: 2, z: 4, core: 2. Of those that a mesh axis runs over, the one named last changes fastest.
Arguments:
- query_rows: bfloat16 [4096, 1024], P('sp', 'tp'), may hold values from -6 to 6
- key_rows: bfloat16 [4096, 1024], P('sp', 'tp'), may hold values from -6 to 6
- value_rows: bfloat16 [4096, 1024], P('sp', 'tp'), may hold values from -6 to 6
- out_weight: bfloat16 [1024, 2048], P('tp'), may hold values from -0.75 to 0.75
Outputs:
- layer_out: bfloat16 [4096, 2048], P(('sp', 'tp'))
The draws below stay inside these ranges and needn't reach their ends.
All inputs are finite; a program needn't handle non-finite values.
Results may differ from the reference program's by a relative error of at most 0.012.
Values may be sent and summed in bfloat16 or wider, within the bound.
A program may use at most 64 MiB of HBM per device.

```python
import math
import jax
import jax.numpy as jnp
from jax import lax

D = 2048
H = 16
HD = 64
BACK = 128
SEQ = 4096


def planted_pair(key):
    base = jax.random.fold_in(key, 11)
    width = H * HD
    first = jnp.clip(jax.random.normal(jax.random.fold_in(base, 1), (SEQ, width), jnp.float32), -6.0, 6.0)
    second = jnp.clip(jax.random.normal(jax.random.fold_in(base, 2), (SEQ, width), jnp.float32), -6.0, 6.0)
    return (first, second)


def draw_query_rows(key, part):
    return planted_pair(key)[0].astype(jnp.bfloat16)


def draw_key_rows(key, part):
    return planted_pair(key)[1].astype(jnp.bfloat16)


def shard_levels(rng, dims, shards, smallest, high):
    factor_of, own = 1.0, jax.random.fold_in(rng, 6)
    for position, blocks in shards:
        heights = jnp.exp(jax.random.uniform(jax.random.fold_in(own, position), (blocks,), jnp.float32, smallest / len(shards), high / len(shards)))
        factor_of = factor_of * jnp.repeat(heights, dims[position] // blocks).reshape([-1 if axis == position else 1 for axis in range(len(dims))])
    return factor_of


def noise(rng, dims, scale, reach, pieces=(), kind=jnp.bfloat16):
    values = jax.random.normal(rng, dims, jnp.float32) * scale
    if len(pieces) > 0:
        values = shard_levels(rng, dims, pieces, -0.22, 0.18) * values
    return jnp.clip(values, min=-reach, max=reach).astype(kind)


def setup_inputs(seed: int = 0) -> dict:
    seeds = jax.random.split(jax.random.key(seed), 5)
    query_rows = draw_query_rows(jax.random.fold_in(seeds[4], 71), 0)
    key_rows = draw_key_rows(jax.random.fold_in(seeds[4], 71), 0)
    value_rows = noise(seeds[2], (SEQ, H * HD), 1.0, 6.0, ((0, 16), (1, 2)))
    out_weight = noise(seeds[3], (H * HD, D), HD ** -0.5, 0.75, ((0, 2),))
    return {"query_rows": query_rows, "key_rows": key_rows, "value_rows": value_rows, "out_weight": out_weight}


THETA = 500000.0
DILATIONS = (1, 4, 16)

def rotate(rows, positions, head_count, head_dim):
    half_dim = head_dim // 2
    inverse = jnp.power(jnp.float32(THETA), -jnp.arange(half_dim, dtype=jnp.float32) / half_dim)
    angles = positions.astype(jnp.float32)[:, None] * inverse[None, :]
    cosine = jnp.cos(angles)[:, None, :]
    sine = jnp.sin(angles)[:, None, :]
    whole = rows.astype(jnp.float32).reshape(rows.shape[0], head_count, head_dim)
    lower = whole[..., :half_dim]
    upper = whole[..., half_dim:]
    turned = jnp.concatenate([lower * cosine - upper * sine, upper * cosine + lower * sine], axis=-1)
    return turned.reshape(rows.shape[0], head_count * head_dim).astype(jnp.bfloat16)

def one_pattern(queries, key_seq, value_seq, dilation):
    head_dim = queries.shape[1]
    length = queries.shape[0] // dilation
    blocks = -(-length // BACK)
    padded = blocks * BACK

    def residue(rows):
        return rows.reshape(length, dilation, head_dim).transpose(1, 0, 2)
    query_sub = jnp.pad(residue(queries), ((0, 0), (0, padded - length), (0, 0)))
    query_sub = query_sub.reshape(dilation, blocks, BACK, head_dim)

    def with_prior(rows):
        extended = jnp.pad(residue(rows), ((0, 0), (BACK, padded - length), (0, 0)))
        prior = extended[:, :padded].reshape(dilation, blocks, BACK, head_dim)
        current = extended[:, BACK:].reshape(dilation, blocks, BACK, head_dim)
        return jnp.concatenate([prior, current], axis=2)
    key_sub = with_prior(key_seq)
    value_sub = with_prior(value_seq)
    scores = jnp.einsum('rnqc,rnkc->rnqk', query_sub.astype(jnp.float32), key_sub.astype(jnp.float32))
    scores = scores * (1.0 / math.sqrt(head_dim))
    query_index = jnp.arange(BACK)[:, None]
    key_index = jnp.arange(2 * BACK)[None, :]
    distance = query_index + BACK - key_index
    key_place = jnp.arange(blocks)[:, None, None] * BACK + key_index[None] - BACK
    allowed = (distance >= 0) & (distance <= BACK) & (key_place >= 0)
    scores = jnp.where(allowed[None], scores, -jnp.inf)
    row_max = lax.optimization_barrier(jnp.max(scores, axis=-1))
    weights = jnp.exp(scores - row_max[..., None])
    row_sum = lax.optimization_barrier(jnp.sum(weights, axis=-1))
    rounded = weights.astype(jnp.bfloat16)
    weighted = jnp.einsum('rnqk,rnkc->rnqc', rounded.astype(jnp.float32), value_sub.astype(jnp.float32))
    result = (weighted / row_sum[..., None]).astype(jnp.bfloat16)
    result = result.reshape(dilation, padded, head_dim)[:, :length].transpose(1, 0, 2)
    result = result.reshape(length * dilation, head_dim)
    row_max = row_max.reshape(dilation, padded)[:, :length].transpose(1, 0).reshape(-1)
    row_sum = row_sum.reshape(dilation, padded)[:, :length].transpose(1, 0).reshape(-1)
    return (result, row_max, row_sum)

def reference(query_rows, key_rows, value_rows, out_weight):
    positions = jnp.arange(SEQ, dtype=jnp.int32)
    turned_q = rotate(query_rows, positions, H, HD)
    turned_k = rotate(key_rows, positions, H, HD)

    def split(rows):
        return rows.reshape(SEQ, H, HD).transpose(1, 0, 2)

    def per_head(stacked):
        query_head, key_head, value_head = stacked
        results, maxima, sums = ([], [], [])
        for dilation in DILATIONS:
            result, row_max, row_sum = one_pattern(query_head, key_head, value_head, dilation)
            results.append(result)
            maxima.append(row_max)
            sums.append(row_sum)
        return (tuple(results), tuple(maxima), tuple(sums))
    results, maxima, sums = lax.map(per_head, (split(turned_q), split(turned_k), split(value_rows)))
    top = jnp.maximum(jnp.maximum(maxima[0], maxima[1]), maxima[2])
    scales = [sums[i] * jnp.exp(maxima[i] - top) for i in range(3)]
    weighted = scales[0][..., None] * results[0].astype(jnp.float32)
    weighted = weighted + scales[1][..., None] * results[1].astype(jnp.float32)
    weighted = weighted + scales[2][..., None] * results[2].astype(jnp.float32)
    denominator = scales[0] + scales[1] + scales[2]
    mixed = weighted / denominator[..., None]
    mixed = mixed.transpose(1, 0, 2).reshape(SEQ, H * HD).astype(jnp.bfloat16)
    return jnp.dot(mixed, out_weight, preferred_element_type=jnp.float32).astype(jnp.bfloat16)
```

```python
import functools
import math

import jax
import jax.numpy as jnp
import numpy as np
from jax import lax
from jax.experimental import pallas as pl
from jax.experimental.pallas import tpu as pltpu
from jax.sharding import PartitionSpec as P

HD = 64
BACK = 128
THETA = 500000.0
FAR = -1e30
F32 = jnp.float32
BF16 = jnp.bfloat16
LANES = 2 * HD
NT = (((1,), (1,)), ((), ()))


def place(p):
    return ((p & 7) << 4) + (((p >> 3) & 3) << 2) + (p >> 5)


def iota(shape, axis):
    return lax.broadcasted_iota(jnp.int32, shape, axis)


def kernel(
    G, ngroups, tp_count,
    q_ref, k_ref, v_ref, cosb_ref, sinb_ref, inv_ref, w_ref, out_ref,
    qs, kvs, qr, kv, kvf, q2, q2f, acc, top, bias, wbuf, rs, rr, mx,
    s_kv, s_q, s_x, r_kv, r_q, r_x, w_sem, s_ret, r_ret,
):
    sp = lax.axis_index("sp")
    tp = lax.axis_index("tp")
    group = sp // G
    me = sp - group * G
    base = group * G
    has_prev = group > 0
    has_next = group < ngroups - 1
    seat = me * tp_count + tp
    seats = G * tp_count
    head = tp * G + me
    tok = q_ref.shape[0]
    halves = tok // BACK

    def target(s, t):
        return {"sp": s, "tp": t}

    barrier = pltpu.get_barrier_semaphore()
    for o in range(1, seats):
        n = lax.rem(seat + o, seats)
        pl.semaphore_signal(
            barrier, inc=1, device_id=target(base + n // tp_count, lax.rem(n, tp_count)),
            device_id_type=pl.DeviceIdType.MESH,
        )

    @pl.when(has_prev)
    def _():
        for o in range(G):
            pl.semaphore_signal(
                barrier, inc=1, device_id=target(base - G + o, tp),
                device_id_type=pl.DeviceIdType.MESH,
            )

    @pl.when(has_next)
    def _():
        for o in range(G):
            pl.semaphore_signal(
                barrier, inc=1, device_id=target(base + G + o, tp),
                device_id_type=pl.DeviceIdType.MESH,
            )

    w_local = pltpu.make_async_copy(w_ref, wbuf.at[tp], w_sem.at[0])
    w_local.start()

    lane = iota((BACK, LANES), 1)
    low = lane < HD
    lane_t = iota((tok, LANES), 1)
    first = (lane_t & (HD - 1)) < HD // 2
    angle = inv_ref[...] * (sp * tok).astype(F32)
    ca = jnp.cos(angle)[:1]
    sa = jnp.sin(angle)[:1]
    cos = ca * cosb_ref[...] - sa * sinb_ref[...]
    sin = sa * cosb_ref[...] + ca * sinb_ref[...]
    sin = jnp.where(first, -sin, sin)
    swizzle = jnp.where(place(iota((BACK, BACK), 0)) == iota((BACK, BACK), 1), 1.0, 0.0).astype(BF16)
    back = jnp.where(place(iota((BACK, BACK), 1)) == iota((BACK, BACK), 0), 1.0, 0.0).astype(BF16)

    def turn(ref, cols):
        x = ref[:, cols].astype(F32)
        other = jnp.where(first, pltpu.roll(x, LANES - HD // 2, 1), pltpu.roll(x, HD // 2, 1))
        return (x * cos + other * sin).astype(BF16)

    def sw(x):
        return jnp.dot(swizzle, x, preferred_element_type=F32)

    for m in range(G // 2):
        cols = slice(m * LANES, (m + 1) * LANES)
        tq = turn(q_ref, cols)
        tk = turn(k_ref, cols)
        tv = v_ref[:, cols]
        qa = sw(tq[:BACK]) * (1.0 / math.sqrt(HD))
        qb = sw(tq[BACK:]) * (1.0 / math.sqrt(HD))
        qs[2 * m] = jnp.where(low, qa, pltpu.roll(qb, HD, 1)).astype(BF16)
        qs[2 * m + 1] = jnp.where(low, pltpu.roll(qa, HD, 1), qb).astype(BF16)
        for e in range(halves):
            ks = sw(tk[e * BACK : (e + 1) * BACK])
            vs = sw(tv[e * BACK : (e + 1) * BACK])
            kvs[2 * m, e] = jnp.where(low, ks, pltpu.roll(vs, HD, 1)).astype(BF16)
            kvs[2 * m + 1, e] = jnp.where(low, pltpu.roll(ks, HD, 1), vs).astype(BF16)

    pl.semaphore_wait(
        barrier, seats - 1 + jnp.where(has_prev, G, 0) + jnp.where(has_next, G, 0)
    )

    own0 = G * halves

    def copy_kv(dest):
        return pltpu.make_async_remote_copy(
            src_ref=kvs.at[dest], dst_ref=kv.at[pl.ds(own0 + halves * me, halves)],
            send_sem=s_kv.at[dest], recv_sem=r_kv.at[me],
            device_id=target(base + dest, tp), device_id_type=pl.DeviceIdType.MESH,
        )

    def copy_q(dest):
        return pltpu.make_async_remote_copy(
            src_ref=qs.at[dest], dst_ref=qr.at[me],
            send_sem=s_q.at[dest], recv_sem=r_q.at[me],
            device_id=target(base + dest, tp), device_id_type=pl.DeviceIdType.MESH,
        )

    def copy_x(dest):
        return pltpu.make_async_remote_copy(
            src_ref=kvs.at[dest], dst_ref=kv.at[pl.ds(halves * me, halves)],
            send_sem=s_x.at[dest], recv_sem=r_x.at[me],
            device_id=target(base + G + dest, tp), device_id_type=pl.DeviceIdType.MESH,
        )

    w_away = pltpu.make_async_remote_copy(
        src_ref=w_ref, dst_ref=wbuf.at[tp], send_sem=w_sem.at[1], recv_sem=w_sem.at[2],
        device_id=target(sp, tp_count - 1 - tp), device_id_type=pl.DeviceIdType.MESH,
    )

    for o in range(1, G):
        copy_kv(lax.rem(me + o, G)).start()
        copy_q(lax.rem(me + o, G)).start()

    @pl.when(has_next)
    def _():
        for o in range(G):
            copy_x(lax.rem(me + o, G)).start()

    w_away.start()

    row = iota((BACK, 2 * BACK), 0)
    col = iota((BACK, 2 * BACK), 1)
    old = col < BACK
    missing = jnp.logical_and(old, group == 0)

    def stride4(n):
        w = n & 31
        return ((n >> 5) << 5) + ((w & 7) << 2) + (w >> 3)

    def masked(distance):
        return jnp.where((distance >= 0) & (distance <= BACK), 0.0, FAR)

    b1 = masked(place(row) + BACK - place(col & (BACK - 1)) - ((col >> 7) << 7))
    b4 = masked(stride4(row) + BACK - stride4(col))
    b16 = masked(row + BACK - col)
    bias[0] = b1
    bias[1] = b4
    bias[2] = jnp.where(missing, FAR, b1)
    bias[3] = jnp.where(missing, FAR, b4)
    bias[4] = jnp.where(missing, FAR, b16)

    acc[...] = jnp.zeros_like(acc)
    top[...] = jnp.full_like(top, FAR)

    @pl.when(jnp.logical_not(has_prev))
    def _():
        kv[:own0] = jnp.zeros((own0, BACK, LANES), BF16)

    kv[pl.ds(own0 + halves * me, halves)] = kvs[me]
    qr[me] = qs[me]

    def ready(s):
        x = qr[s].astype(F32)
        a = jnp.where(low, x, 0.0)
        b = jnp.where(low, pltpu.roll(x, HD, 1), 0.0)
        q2f[2 * s] = a
        q2f[2 * s + 1] = b
        q2[2 * s] = a.astype(BF16)
        q2[2 * s + 1] = b.astype(BF16)
        at = pl.ds(own0 + halves * s, halves)
        kvf[at] = kv[at].astype(F32)

    ready(me)
    for o in range(1, G):
        s = lax.rem(me - o + G, G)
        pltpu.make_async_remote_copy(
            src_ref=kvs.at[s], dst_ref=kv.at[pl.ds(own0 + halves * s, halves)],
            send_sem=s_kv.at[s], recv_sem=r_kv.at[s],
            device_id=target(base + s, tp), device_id_type=pl.DeviceIdType.MESH,
        ).wait_recv()
        pltpu.make_async_remote_copy(
            src_ref=qs.at[s], dst_ref=qr.at[s],
            send_sem=s_q.at[s], recv_sem=r_q.at[s],
            device_id=target(base + s, tp), device_id_type=pl.DeviceIdType.MESH,
        ).wait_recv()
        ready(s)

    low_keys = iota((2 * BACK, LANES), 1) < HD

    def attend(q, keys, b, o_old, t_old):
        s = lax.dot_general(q, keys, NT, preferred_element_type=F32) + b
        t_new = jnp.maximum(t_old, jnp.max(s, axis=1, keepdims=True))
        p = jnp.concatenate(
            [jnp.exp(s[:, :BACK] - t_new), jnp.exp(s[:, BACK:] - t_new)], axis=1
        ).astype(BF16)
        ones = jnp.where(low_keys, jnp.ones_like(keys), keys)
        o = jnp.dot(p, ones, preferred_element_type=F32)
        return o_old * jnp.exp(t_old - t_new) + o, t_new

    def run(tiles):
        done = []
        for q, keys, b, where in tiles:
            shape = acc[where].shape
            o, t = attend(
                q, keys, b, acc[where].reshape(BACK, LANES), top[where].reshape(BACK, LANES)
            )
            done.append((where, o.reshape(shape), t.reshape(shape)))
        for where, o, t in done:
            acc[where] = o
            top[where] = t

    def tile1(h, b):
        return (
            q2[h], kv[pl.ds(own0 - 1 + h, 2)].reshape(2 * BACK, LANES), bias[b], (h,),
        )

    def tile4(quarter, r, b):
        rows = pl.ds(r * 32, 32)
        return (
            q2[4 * quarter : 4 * quarter + 4, rows, :].reshape(BACK, LANES),
            kv[own0 + 4 * quarter - 4 : own0 + 4 * quarter + 4, rows, :].reshape(2 * BACK, LANES),
            bias[b],
            (slice(4 * quarter, 4 * quarter + 4), rows, slice(None)),
        )

    def tile16(r):
        rows = pl.ds(r * 8, 8)
        return (
            q2f[:, rows, :].reshape(BACK, LANES).astype(BF16),
            kvf[:, rows, :].reshape(2 * BACK, LANES).astype(BF16),
            bias[4],
            (slice(None), rows, slice(None)),
        )

    nq = G * halves

    @pl.loop(0, (nq - 1) // 3)
    def _(i):
        run([tile1(1 + 3 * i + n, 0) for n in range(3)])

    @pl.loop(0, 4)
    def _(r):
        run([tile4(n, r, 1) for n in range(1, nq // 4)])

    @pl.when(has_prev)
    def _():
        for o in range(G):
            s = lax.rem(me - o + G, G)
            pltpu.make_async_remote_copy(
                src_ref=kvs.at[s], dst_ref=kv.at[pl.ds(halves * s, halves)],
                send_sem=s_x.at[s], recv_sem=r_x.at[s],
                device_id=target(base - G + s, tp), device_id_type=pl.DeviceIdType.MESH,
            ).wait_recv()

    @pl.loop(0, G)
    def _(i):
        at = pl.ds(2 * i, 2)
        kvf[at] = kv[at].astype(F32)

    run([tile1(0, 2)])
    run([tile4(0, r, 3) for r in range(4)])

    @pl.loop(0, 4)
    def _(i):
        run([tile16(4 * i + n) for n in range(4)])

    @pl.loop(0, nq)
    def _(h):
        o = acc[h]
        y = o / pltpu.roll(o, HD, 1)
        rs[h] = jnp.where(low[: HD], pltpu.roll(y[:HD], HD, 1), y[HD:]).astype(BF16)

    def copy_ret(n):
        return pltpu.make_async_remote_copy(
            src_ref=rs.at[n], dst_ref=rr.at[head], send_sem=s_ret.at[n], recv_sem=r_ret.at[head],
            device_id=target(base + n // tp_count, lax.rem(n, tp_count)),
            device_id_type=pl.DeviceIdType.MESH,
        )

    for o in range(1, seats):
        copy_ret(lax.rem(seat + o, seats)).start()
    rr[head] = rs[seat]

    for o in range(1, G):
        copy_kv(lax.rem(me + o, G)).wait_send()
        copy_q(lax.rem(me + o, G)).wait_send()

    @pl.when(has_next)
    def _():
        for o in range(G):
            copy_x(lax.rem(me + o, G)).wait_send()

    w_local.wait()
    w_away.wait_send()
    pltpu.make_async_remote_copy(
        src_ref=w_ref, dst_ref=wbuf.at[tp_count - 1 - tp],
        send_sem=w_sem.at[1], recv_sem=w_sem.at[2],
        device_id=target(sp, tp_count - 1 - tp), device_id_type=pl.DeviceIdType.MESH,
    ).wait_recv()

    for o in range(1, seats):
        n = lax.rem(seat - o + seats, seats)
        their = lax.rem(n, tp_count) * G + n // tp_count
        pltpu.make_async_remote_copy(
            src_ref=rs.at[n], dst_ref=rr.at[their], send_sem=s_ret.at[n],
            recv_sem=r_ret.at[their],
            device_id=target(base + n // tp_count, lax.rem(n, tp_count)),
            device_id_type=pl.DeviceIdType.MESH,
        ).wait_recv()

    low_h = low[:HD]
    for m in range(seats // 2):
        x0 = rr[2 * m].astype(F32)
        x1 = rr[2 * m + 1].astype(F32)
        pair = jnp.concatenate(
            [jnp.where(low_h, x0, pltpu.roll(x1, HD, 1)), jnp.where(low_h, pltpu.roll(x0, HD, 1), x1)],
            axis=0,
        ).astype(BF16)
        mx[:, m * LANES : (m + 1) * LANES] = jnp.dot(
            back, pair, preferred_element_type=F32
        ).astype(BF16)

    width = wbuf.shape[1]
    step = 512

    @pl.loop(0, out_ref.shape[1] // step)
    def _(c):
        cols = pl.ds(pl.multiple_of(c * step, step), step)
        total = jnp.dot(mx[:, :width], wbuf[0, :, cols], preferred_element_type=F32)
        total = total + jnp.dot(mx[:, width:], wbuf[1, :, cols], preferred_element_type=F32)
        out_ref[:, cols] = total.astype(BF16)

    for o in range(1, seats):
        copy_ret(lax.rem(seat + o, seats)).wait_send()


def per_device(sp_count, tp_count, query_rows, key_rows, value_rows, out_weight):
    tok = query_rows.shape[0]
    G = query_rows.shape[1] // HD
    halves = tok // BACK
    ngroups = sp_count // G
    assert tok == 2 * BACK and tp_count == 2 and sp_count % G == 0
    assert G * tok == 16 * BACK
    inverse = np.power(THETA, -np.arange(HD // 2) / (HD // 2))
    inverse = np.tile(inverse, LANES // (HD // 2))[None, :]
    local = np.arange(tok)[:, None] * inverse
    cosb = jnp.asarray(np.cos(local), F32)
    sinb = jnp.asarray(np.sin(local), F32)
    inv = jnp.asarray(np.tile(inverse, (8, 1)), F32)
    seats = G * tp_count
    vmem = pl.BlockSpec(memory_space=pltpu.VMEM)
    dma = pltpu.SemaphoreType.DMA
    return pl.pallas_call(
        functools.partial(kernel, G, ngroups, tp_count),
        out_shape=jax.ShapeDtypeStruct((tok // tp_count, out_weight.shape[1]), BF16),
        in_specs=[vmem] * 6 + [pl.BlockSpec(memory_space=pl.ANY)],
        out_specs=vmem,
        scratch_shapes=[
            pltpu.VMEM((G, BACK, LANES), BF16),
            pltpu.VMEM((G, halves, BACK, LANES), BF16),
            pltpu.VMEM((G, BACK, LANES), BF16),
            pltpu.VMEM((2 * G * halves, BACK, LANES), BF16),
            pltpu.VMEM((2 * G * halves, BACK, LANES), F32),
            pltpu.VMEM((G * halves, BACK, LANES), BF16),
            pltpu.VMEM((G * halves, BACK, LANES), F32),
            pltpu.VMEM((G * halves, BACK, LANES), F32),
            pltpu.VMEM((G * halves, BACK, LANES), F32),
            pltpu.VMEM((5, BACK, 2 * BACK), F32),
            pltpu.VMEM((tp_count,) + out_weight.shape, BF16),
            pltpu.VMEM((seats, HD, LANES), BF16),
            pltpu.VMEM((seats, HD, LANES), BF16),
            pltpu.VMEM((BACK, seats * HD), BF16),
            dma((G,)), dma((G,)), dma((G,)), dma((G,)), dma((G,)), dma((G,)),
            dma((3,)), dma((seats,)), dma((seats,)),
        ],
        compiler_params=pltpu.CompilerParams(
            collective_id=0, has_side_effects=True, vmem_limit_bytes=48 * 1024 * 1024
        ),
    )(query_rows, key_rows, value_rows, cosb, sinb, inv, out_weight)


def solution(mesh):
    return jax.shard_map(
        functools.partial(per_device, mesh.shape["sp"], mesh.shape["tp"]),
        mesh=mesh,
        in_specs=(P("sp", "tp"), P("sp", "tp"), P("sp", "tp"), P("tp", None)),
        out_specs=P(("sp", "tp"), None),
        check_vma=False,
    )
```

```python
import functools
import math

import jax
import jax.numpy as jnp
import numpy as np
from jax import lax
from jax.experimental import pallas as pl
from jax.experimental.pallas import tpu as pltpu
from jax.sharding import PartitionSpec as P

HD = 64
BACK = 128
THETA = 500000.0
FAR = -1e30
F32 = jnp.float32
BF16 = jnp.bfloat16
LANES = 2 * HD
NT = (((1,), (1,)), ((), ()))


def place(p):
    return ((p & 7) << 4) + (((p >> 3) & 3) << 2) + (p >> 5)


def iota(shape, axis):
    return lax.broadcasted_iota(jnp.int32, shape, axis)


def kernel(
    G, ngroups, tp_count,
    q_hbm, k_hbm, v_hbm, cosb_hbm, sinb_hbm, inv_hbm, w_ref, out_ref,
    q_ref, k_ref, v_ref, cosb_ref, sinb_ref, inv_ref, qs, kvs, qr, kv, kvf, q2, q2f, acc, top, bias, wbuf, rs, rr, mx,
    s_kv, s_q, s_x, r_kv, r_q, r_x, w_sem, s_ret, r_ret, in_sem,
):
    loads = [
        pltpu.make_async_copy(source, dest, in_sem.at[n])
        for n, (source, dest) in enumerate((
            (inv_hbm, inv_ref), (cosb_hbm, cosb_ref), (sinb_hbm, sinb_ref),
            (k_hbm, k_ref), (v_hbm, v_ref), (q_hbm, q_ref),
        ))
    ]
    for load in loads:
        load.start()
    sp = lax.axis_index("sp")
    tp = lax.axis_index("tp")
    group = sp // G
    me = sp - group * G
    base = group * G
    has_prev = group > 0
    has_next = group < ngroups - 1
    seat = me * tp_count + tp
    seats = G * tp_count
    head = tp * G + me
    tok = q_ref.shape[0]
    halves = tok // BACK

    def target(s, t):
        return {"sp": s, "tp": t}

    barrier = pltpu.get_barrier_semaphore()
    for o in range(1, seats):
        n = lax.rem(seat + o, seats)
        pl.semaphore_signal(
            barrier, inc=1, device_id=target(base + n // tp_count, lax.rem(n, tp_count)),
            device_id_type=pl.DeviceIdType.MESH,
        )

    @pl.when(has_prev)
    def _():
        for o in range(G):
            pl.semaphore_signal(
                barrier, inc=1, device_id=target(base - G + o, tp),
                device_id_type=pl.DeviceIdType.MESH,
            )

    @pl.when(has_next)
    def _():
        for o in range(G):
            pl.semaphore_signal(
                barrier, inc=1, device_id=target(base + G + o, tp),
                device_id_type=pl.DeviceIdType.MESH,
            )

    w_local = pltpu.make_async_copy(w_ref, wbuf.at[tp], w_sem.at[0])
    w_local.start()

    for load in loads:
        load.wait()

    lane = iota((BACK, LANES), 1)
    low = lane < HD
    lane_t = iota((tok, LANES), 1)
    first = (lane_t & (HD - 1)) < HD // 2
    angle = inv_ref[...] * (sp * tok).astype(F32)
    ca = jnp.cos(angle)[:1]
    sa = jnp.sin(angle)[:1]
    cos = ca * cosb_ref[...] - sa * sinb_ref[...]
    sin = sa * cosb_ref[...] + ca * sinb_ref[...]
    sin = jnp.where(first, -sin, sin)
    swizzle = jnp.where(place(iota((BACK, BACK), 0)) == iota((BACK, BACK), 1), 1.0, 0.0).astype(BF16)
    back = jnp.where(place(iota((BACK, BACK), 1)) == iota((BACK, BACK), 0), 1.0, 0.0).astype(BF16)

    def turn(ref, cols):
        x = ref[:, cols].astype(F32)
        other = jnp.where(first, pltpu.roll(x, LANES - HD // 2, 1), pltpu.roll(x, HD // 2, 1))
        return (x * cos + other * sin).astype(BF16)

    def sw(x):
        return jnp.dot(swizzle, x, preferred_element_type=F32)

    for m in range(G // 2):
        cols = slice(m * LANES, (m + 1) * LANES)
        tq = turn(q_ref, cols)
        tk = turn(k_ref, cols)
        tv = v_ref[:, cols]
        qa = sw(tq[:BACK]) * (1.0 / math.sqrt(HD))
        qb = sw(tq[BACK:]) * (1.0 / math.sqrt(HD))
        qs[2 * m] = jnp.where(low, qa, pltpu.roll(qb, HD, 1)).astype(BF16)
        qs[2 * m + 1] = jnp.where(low, pltpu.roll(qa, HD, 1), qb).astype(BF16)
        for e in range(halves):
            ks = sw(tk[e * BACK : (e + 1) * BACK])
            vs = sw(tv[e * BACK : (e + 1) * BACK])
            kvs[2 * m, e] = jnp.where(low, ks, pltpu.roll(vs, HD, 1)).astype(BF16)
            kvs[2 * m + 1, e] = jnp.where(low, pltpu.roll(ks, HD, 1), vs).astype(BF16)

    pl.semaphore_wait(
        barrier, seats - 1 + jnp.where(has_prev, G, 0) + jnp.where(has_next, G, 0)
    )

    own0 = G * halves

    def copy_kv(dest):
        return pltpu.make_async_remote_copy(
            src_ref=kvs.at[dest], dst_ref=kv.at[pl.ds(own0 + halves * me, halves)],
            send_sem=s_kv.at[dest], recv_sem=r_kv.at[me],
            device_id=target(base + dest, tp), device_id_type=pl.DeviceIdType.MESH,
        )

    def copy_q(dest):
        return pltpu.make_async_remote_copy(
            src_ref=qs.at[dest], dst_ref=qr.at[me],
            send_sem=s_q.at[dest], recv_sem=r_q.at[me],
            device_id=target(base + dest, tp), device_id_type=pl.DeviceIdType.MESH,
        )

    def copy_x(dest):
        return pltpu.make_async_remote_copy(
            src_ref=kvs.at[dest], dst_ref=kv.at[pl.ds(halves * me, halves)],
            send_sem=s_x.at[dest], recv_sem=r_x.at[me],
            device_id=target(base + G + dest, tp), device_id_type=pl.DeviceIdType.MESH,
        )

    w_away = pltpu.make_async_remote_copy(
        src_ref=w_ref, dst_ref=wbuf.at[tp], send_sem=w_sem.at[1], recv_sem=w_sem.at[2],
        device_id=target(sp, tp_count - 1 - tp), device_id_type=pl.DeviceIdType.MESH,
    )

    for o in range(1, G):
        copy_kv(lax.rem(me + o, G)).start()
        copy_q(lax.rem(me + o, G)).start()

    @pl.when(has_next)
    def _():
        for o in range(G):
            copy_x(lax.rem(me + o, G)).start()

    w_away.start()

    row = iota((BACK, 2 * BACK), 0)
    col = iota((BACK, 2 * BACK), 1)
    old = col < BACK
    missing = jnp.logical_and(old, group == 0)

    def stride4(n):
        w = n & 31
        return ((n >> 5) << 5) + ((w & 7) << 2) + (w >> 3)

    def masked(distance):
        return jnp.where((distance >= 0) & (distance <= BACK), 0.0, FAR)

    b1 = masked(place(row) + BACK - place(col & (BACK - 1)) - ((col >> 7) << 7))
    b4 = masked(stride4(row) + BACK - stride4(col))
    b16 = masked(row + BACK - col)
    bias[0] = b1
    bias[1] = b4
    bias[2] = jnp.where(missing, FAR, b1)
    bias[3] = jnp.where(missing, FAR, b4)
    bias[4] = jnp.where(missing, FAR, b16)

    acc[...] = jnp.zeros_like(acc)
    top[...] = jnp.full_like(top, FAR)

    @pl.when(jnp.logical_not(has_prev))
    def _():
        kv[:own0] = jnp.zeros((own0, BACK, LANES), BF16)

    kv[pl.ds(own0 + halves * me, halves)] = kvs[me]
    qr[me] = qs[me]

    def ready(s):
        x = qr[s].astype(F32)
        a = jnp.where(low, x, 0.0)
        b = jnp.where(low, pltpu.roll(x, HD, 1), 0.0)
        q2f[2 * s] = a
        q2f[2 * s + 1] = b
        q2[2 * s] = a.astype(BF16)
        q2[2 * s + 1] = b.astype(BF16)
        at = pl.ds(own0 + halves * s, halves)
        kvf[at] = kv[at].astype(F32)

    ready(me)
    for o in range(1, G):
        s = lax.rem(me - o + G, G)
        pltpu.make_async_remote_copy(
            src_ref=kvs.at[s], dst_ref=kv.at[pl.ds(own0 + halves * s, halves)],
            send_sem=s_kv.at[s], recv_sem=r_kv.at[s],
            device_id=target(base + s, tp), device_id_type=pl.DeviceIdType.MESH,
        ).wait_recv()
        pltpu.make_async_remote_copy(
            src_ref=qs.at[s], dst_ref=qr.at[s],
            send_sem=s_q.at[s], recv_sem=r_q.at[s],
            device_id=target(base + s, tp), device_id_type=pl.DeviceIdType.MESH,
        ).wait_recv()
        ready(s)

    low_keys = iota((2 * BACK, LANES), 1) < HD

    def attend(q, keys, b, o_old, t_old):
        s = lax.dot_general(q, keys, NT, preferred_element_type=F32) + b
        t_new = jnp.maximum(t_old, jnp.max(s, axis=1, keepdims=True))
        p = jnp.concatenate(
            [jnp.exp(s[:, :BACK] - t_new), jnp.exp(s[:, BACK:] - t_new)], axis=1
        ).astype(BF16)
        ones = jnp.where(low_keys, jnp.ones_like(keys), keys)
        o = jnp.dot(p, ones, preferred_element_type=F32)
        return o_old * jnp.exp(t_old - t_new) + o, t_new

    def run(tiles):
        done = []
        for q, keys, b, where in tiles:
            shape = acc[where].shape
            o, t = attend(
                q, keys, b, acc[where].reshape(BACK, LANES), top[where].reshape(BACK, LANES)
            )
            done.append((where, o.reshape(shape), t.reshape(shape)))
        for where, o, t in done:
            acc[where] = o
            top[where] = t

    def tile1(h, b):
        return (
            q2[h], kv[pl.ds(own0 - 1 + h, 2)].reshape(2 * BACK, LANES), bias[b], (h,),
        )

    def tile4(quarter, r, b):
        rows = pl.ds(r * 32, 32)
        return (
            q2[4 * quarter : 4 * quarter + 4, rows, :].reshape(BACK, LANES),
            kv[own0 + 4 * quarter - 4 : own0 + 4 * quarter + 4, rows, :].reshape(2 * BACK, LANES),
            bias[b],
            (slice(4 * quarter, 4 * quarter + 4), rows, slice(None)),
        )

    def tile16(r):
        rows = pl.ds(r * 8, 8)
        return (
            q2f[:, rows, :].reshape(BACK, LANES).astype(BF16),
            kvf[:, rows, :].reshape(2 * BACK, LANES).astype(BF16),
            bias[4],
            (slice(None), rows, slice(None)),
        )

    nq = G * halves

    @pl.loop(0, (nq - 1) // 3)
    def _(i):
        run([tile1(1 + 3 * i + n, 0) for n in range(3)])

    @pl.loop(0, 4)
    def _(r):
        run([tile4(n, r, 1) for n in range(1, nq // 4)])

    @pl.when(has_prev)
    def _():
        for o in range(G):
            s = lax.rem(me - o + G, G)
            pltpu.make_async_remote_copy(
                src_ref=kvs.at[s], dst_ref=kv.at[pl.ds(halves * s, halves)],
                send_sem=s_x.at[s], recv_sem=r_x.at[s],
                device_id=target(base - G + s, tp), device_id_type=pl.DeviceIdType.MESH,
            ).wait_recv()

    @pl.loop(0, G)
    def _(i):
        at = pl.ds(2 * i, 2)
        kvf[at] = kv[at].astype(F32)

    run([tile1(0, 2)])
    run([tile4(0, r, 3) for r in range(4)])

    @pl.loop(0, 4)
    def _(i):
        run([tile16(4 * i + n) for n in range(4)])

    @pl.loop(0, nq)
    def _(h):
        o = acc[h]
        y = o / pltpu.roll(o, HD, 1)
        rs[h] = jnp.where(low[: HD], pltpu.roll(y[:HD], HD, 1), y[HD:]).astype(BF16)

    def copy_ret(n):
        return pltpu.make_async_remote_copy(
            src_ref=rs.at[n], dst_ref=rr.at[head], send_sem=s_ret.at[n], recv_sem=r_ret.at[head],
            device_id=target(base + n // tp_count, lax.rem(n, tp_count)),
            device_id_type=pl.DeviceIdType.MESH,
        )

    for o in range(1, seats):
        copy_ret(lax.rem(seat + o, seats)).start()
    rr[head] = rs[seat]

    for o in range(1, G):
        copy_kv(lax.rem(me + o, G)).wait_send()
        copy_q(lax.rem(me + o, G)).wait_send()

    @pl.when(has_next)
    def _():
        for o in range(G):
            copy_x(lax.rem(me + o, G)).wait_send()

    w_local.wait()
    w_away.wait_send()
    pltpu.make_async_remote_copy(
        src_ref=w_ref, dst_ref=wbuf.at[tp_count - 1 - tp],
        send_sem=w_sem.at[1], recv_sem=w_sem.at[2],
        device_id=target(sp, tp_count - 1 - tp), device_id_type=pl.DeviceIdType.MESH,
    ).wait_recv()

    for o in range(1, seats):
        n = lax.rem(seat - o + seats, seats)
        their = lax.rem(n, tp_count) * G + n // tp_count
        pltpu.make_async_remote_copy(
            src_ref=rs.at[n], dst_ref=rr.at[their], send_sem=s_ret.at[n],
            recv_sem=r_ret.at[their],
            device_id=target(base + n // tp_count, lax.rem(n, tp_count)),
            device_id_type=pl.DeviceIdType.MESH,
        ).wait_recv()

    low_h = low[:HD]
    for m in range(seats // 2):
        x0 = rr[2 * m].astype(F32)
        x1 = rr[2 * m + 1].astype(F32)
        pair = jnp.concatenate(
            [jnp.where(low_h, x0, pltpu.roll(x1, HD, 1)), jnp.where(low_h, pltpu.roll(x0, HD, 1), x1)],
            axis=0,
        ).astype(BF16)
        mx[:, m * LANES : (m + 1) * LANES] = jnp.dot(
            back, pair, preferred_element_type=F32
        ).astype(BF16)

    width = wbuf.shape[1]
    step = 512

    @pl.loop(0, out_ref.shape[1] // step)
    def _(c):
        cols = pl.ds(pl.multiple_of(c * step, step), step)
        total = jnp.dot(mx[:, :width], wbuf[0, :, cols], preferred_element_type=F32)
        total = total + jnp.dot(mx[:, width:], wbuf[1, :, cols], preferred_element_type=F32)
        out_ref[:, cols] = total.astype(BF16)

    for o in range(1, seats):
        copy_ret(lax.rem(seat + o, seats)).wait_send()


def per_device(sp_count, tp_count, query_rows, key_rows, value_rows, out_weight):
    tok = query_rows.shape[0]
    G = query_rows.shape[1] // HD
    halves = tok // BACK
    ngroups = sp_count // G
    assert tok == 2 * BACK and tp_count == 2 and sp_count % G == 0
    assert G * tok == 16 * BACK
    inverse = np.power(THETA, -np.arange(HD // 2) / (HD // 2))
    inverse = np.tile(inverse, LANES // (HD // 2))[None, :]
    local = np.arange(tok)[:, None] * inverse
    cosb = jnp.asarray(np.cos(local), F32)
    sinb = jnp.asarray(np.sin(local), F32)
    inv = jnp.asarray(np.tile(inverse, (8, 1)), F32)
    seats = G * tp_count
    vmem = pl.BlockSpec(memory_space=pltpu.VMEM)
    dma = pltpu.SemaphoreType.DMA
    return pl.pallas_call(
        functools.partial(kernel, G, ngroups, tp_count),
        out_shape=jax.ShapeDtypeStruct((tok // tp_count, out_weight.shape[1]), BF16),
        in_specs=[pl.BlockSpec(memory_space=pl.ANY)] * 7,
        out_specs=vmem,
        scratch_shapes=[
            pltpu.VMEM(query_rows.shape, BF16),
            pltpu.VMEM(query_rows.shape, BF16),
            pltpu.VMEM(query_rows.shape, BF16),
            pltpu.VMEM(cosb.shape, F32),
            pltpu.VMEM(sinb.shape, F32),
            pltpu.VMEM(inv.shape, F32),
            pltpu.VMEM((G, BACK, LANES), BF16),
            pltpu.VMEM((G, halves, BACK, LANES), BF16),
            pltpu.VMEM((G, BACK, LANES), BF16),
            pltpu.VMEM((2 * G * halves, BACK, LANES), BF16),
            pltpu.VMEM((2 * G * halves, BACK, LANES), F32),
            pltpu.VMEM((G * halves, BACK, LANES), BF16),
            pltpu.VMEM((G * halves, BACK, LANES), F32),
            pltpu.VMEM((G * halves, BACK, LANES), F32),
            pltpu.VMEM((G * halves, BACK, LANES), F32),
            pltpu.VMEM((5, BACK, 2 * BACK), F32),
            pltpu.VMEM((tp_count,) + out_weight.shape, BF16),
            pltpu.VMEM((seats, HD, LANES), BF16),
            pltpu.VMEM((seats, HD, LANES), BF16),
            pltpu.VMEM((BACK, seats * HD), BF16),
            dma((G,)), dma((G,)), dma((G,)), dma((G,)), dma((G,)), dma((G,)),
            dma((3,)), dma((seats,)), dma((seats,)), dma((6,)),
        ],
        compiler_params=pltpu.CompilerParams(
            collective_id=0, has_side_effects=True, vmem_limit_bytes=63 * 1024 * 1024
        ),
    )(query_rows, key_rows, value_rows, cosb, sinb, inv, out_weight)


def solution(mesh):
    return jax.shard_map(
        functools.partial(per_device, mesh.shape["sp"], mesh.shape["tp"]),
        mesh=mesh,
        in_specs=(P("sp", "tp"), P("sp", "tp"), P("sp", "tp"), P("tp", None)),
        out_specs=P(("sp", "tp"), None),
        check_vma=False,
    )
```

```python
import functools
import math

import jax
import jax.numpy as jnp
import numpy as np
from jax import lax
from jax.experimental import pallas as pl
from jax.experimental.pallas import tpu as pltpu
from jax.sharding import PartitionSpec as P

HD = 64
BACK = 128
THETA = 500000.0
FAR = -1e30
F32 = jnp.float32
BF16 = jnp.bfloat16
LANES = 2 * HD
NT = (((1,), (1,)), ((), ()))


def place(p):
    return ((p & 7) << 4) + (((p >> 3) & 3) << 2) + (p >> 5)


def iota(shape, axis):
    return lax.broadcasted_iota(jnp.int32, shape, axis)


def kernel(
    G, ngroups, tp_count,
    q_hbm, k_hbm, v_hbm, cosb_hbm, sinb_hbm, inv_hbm, w_ref, out_ref,
    q_ref, k_ref, v_ref, cosb_ref, sinb_ref, inv_ref, qs, kvs, qr, kv, kvf, q2, q2f, acc, top, bias, wbuf, rs, rr, mx,
    s_kv, s_q, s_x, r_kv, r_q, r_x, w_sem, s_ret, r_ret, in_sem,
):
    loads = [
        pltpu.make_async_copy(source, dest, in_sem.at[n])
        for n, (source, dest) in enumerate((
            (inv_hbm, inv_ref), (cosb_hbm, cosb_ref), (sinb_hbm, sinb_ref),
            (k_hbm, k_ref), (v_hbm, v_ref), (q_hbm, q_ref),
        ))
    ]
    for load in loads:
        load.start()
    sp = lax.axis_index("sp")
    tp = lax.axis_index("tp")
    group = sp // G
    me = sp - group * G
    base = group * G
    has_prev = group > 0
    has_next = group < ngroups - 1
    seat = me * tp_count + tp
    seats = G * tp_count
    head = tp * G + me
    tok = q_ref.shape[0]
    halves = tok // BACK

    def target(s, t):
        return {"sp": s, "tp": t}

    barrier = pltpu.get_barrier_semaphore()
    for o in range(1, seats):
        n = lax.rem(seat + o, seats)
        pl.semaphore_signal(
            barrier, inc=1, device_id=target(base + n // tp_count, lax.rem(n, tp_count)),
            device_id_type=pl.DeviceIdType.MESH,
        )

    @pl.when(has_prev)
    def _():
        for o in range(G):
            pl.semaphore_signal(
                barrier, inc=1, device_id=target(base - G + o, tp),
                device_id_type=pl.DeviceIdType.MESH,
            )

    @pl.when(has_next)
    def _():
        for o in range(G):
            pl.semaphore_signal(
                barrier, inc=1, device_id=target(base + G + o, tp),
                device_id_type=pl.DeviceIdType.MESH,
            )

    w_local = pltpu.make_async_copy(w_ref, wbuf.at[tp], w_sem.at[0])
    w_local.start()

    for load in loads:
        load.wait()

    lane = iota((BACK, LANES), 1)
    low = lane < HD
    lane_t = iota((tok, LANES), 1)
    first = (lane_t & (HD - 1)) < HD // 2
    angle = inv_ref[...] * (sp * tok).astype(F32)
    ca = jnp.cos(angle)[:1]
    sa = jnp.sin(angle)[:1]
    cos = ca * cosb_ref[...] - sa * sinb_ref[...]
    sin = sa * cosb_ref[...] + ca * sinb_ref[...]
    sin = jnp.where(first, -sin, sin)
    swizzle = jnp.where(place(iota((BACK, BACK), 0)) == iota((BACK, BACK), 1), 1.0, 0.0).astype(BF16)
    back = jnp.where(place(iota((BACK, BACK), 1)) == iota((BACK, BACK), 0), 1.0, 0.0).astype(BF16)

    def turn(ref, cols):
        x = ref[:, cols].astype(F32)
        other = jnp.where(first, pltpu.roll(x, LANES - HD // 2, 1), pltpu.roll(x, HD // 2, 1))
        return (x * cos + other * sin).astype(BF16)

    def sw(x):
        return jnp.dot(swizzle, x, preferred_element_type=F32)

    own0 = G * halves

    def copy_kv(dest):
        return pltpu.make_async_remote_copy(
            src_ref=kvs.at[dest], dst_ref=kv.at[pl.ds(own0 + halves * me, halves)],
            send_sem=s_kv.at[dest], recv_sem=r_kv.at[me],
            device_id=target(base + dest, tp), device_id_type=pl.DeviceIdType.MESH,
        )

    def copy_q(dest):
        return pltpu.make_async_remote_copy(
            src_ref=qs.at[dest], dst_ref=qr.at[me],
            send_sem=s_q.at[dest], recv_sem=r_q.at[me],
            device_id=target(base + dest, tp), device_id_type=pl.DeviceIdType.MESH,
        )

    def copy_x(dest):
        return pltpu.make_async_remote_copy(
            src_ref=kvs.at[dest], dst_ref=kv.at[pl.ds(halves * me, halves)],
            send_sem=s_x.at[dest], recv_sem=r_x.at[me],
            device_id=target(base + G + dest, tp), device_id_type=pl.DeviceIdType.MESH,
        )

    w_away = pltpu.make_async_remote_copy(
        src_ref=w_ref, dst_ref=wbuf.at[tp], send_sem=w_sem.at[1], recv_sem=w_sem.at[2],
        device_id=target(sp, tp_count - 1 - tp), device_id_type=pl.DeviceIdType.MESH,
    )

    pairs = G // 2

    def send(m):
        for d in (2 * m, 2 * m + 1):

            @pl.when(has_next)
            def _():
                copy_x(d).start()

            @pl.when(d != me)
            def _():
                copy_kv(d).start()
                copy_q(d).start()

    for i in range(pairs):
        m = lax.rem(me // 2 + i + 1, pairs)
        cols = pl.ds(pl.multiple_of(m * LANES, LANES), LANES)
        tq = turn(q_ref, cols)
        tk = turn(k_ref, cols)
        tv = v_ref[:, cols]
        qa = sw(tq[:BACK]) * (1.0 / math.sqrt(HD))
        qb = sw(tq[BACK:]) * (1.0 / math.sqrt(HD))
        qs[2 * m] = jnp.where(low, qa, pltpu.roll(qb, HD, 1)).astype(BF16)
        qs[2 * m + 1] = jnp.where(low, pltpu.roll(qa, HD, 1), qb).astype(BF16)
        for e in range(halves):
            ks = sw(tk[e * BACK : (e + 1) * BACK])
            vs = sw(tv[e * BACK : (e + 1) * BACK])
            kvs[2 * m, e] = jnp.where(low, ks, pltpu.roll(vs, HD, 1)).astype(BF16)
            kvs[2 * m + 1, e] = jnp.where(low, pltpu.roll(ks, HD, 1), vs).astype(BF16)
        if i == 0:
            pl.semaphore_wait(
                barrier, seats - 1 + jnp.where(has_prev, G, 0) + jnp.where(has_next, G, 0)
            )
        else:
            send(lax.rem(me // 2 + i, pairs))
    send(lax.rem(me // 2 + pairs, pairs))
    w_away.start()

    row = iota((BACK, 2 * BACK), 0)
    col = iota((BACK, 2 * BACK), 1)
    def stride4(n):
        w = n & 31
        return ((n >> 5) << 5) + ((w & 7) << 2) + (w >> 3)

    def masked(distance):
        return jnp.where((distance >= 0) & (distance <= BACK), 0.0, FAR)

    b1 = masked(place(row) + BACK - place(col & (BACK - 1)) - ((col >> 7) << 7))
    b4 = masked(stride4(row) + BACK - stride4(col))
    b16 = masked(row + BACK - col)
    bias[0] = b1
    bias[1] = b4
    bias[2] = b16

    acc[...] = jnp.zeros_like(acc)
    top[...] = jnp.full_like(top, FAR)

    kv[pl.ds(own0 + halves * me, halves)] = kvs[me]
    qr[me] = qs[me]

    def ready(s):
        x = qr[s].astype(F32)
        a = jnp.where(low, x, 0.0)
        b = jnp.where(low, pltpu.roll(x, HD, 1), 0.0)
        q2f[2 * s] = a
        q2f[2 * s + 1] = b
        q2[2 * s] = a.astype(BF16)
        q2[2 * s + 1] = b.astype(BF16)
        at = pl.ds(own0 + halves * s, halves)
        kvf[at] = kv[at].astype(F32)

    ready(me)
    for o in range(1, G):
        s = lax.rem(me - o + G, G)
        pltpu.make_async_remote_copy(
            src_ref=kvs.at[s], dst_ref=kv.at[pl.ds(own0 + halves * s, halves)],
            send_sem=s_kv.at[s], recv_sem=r_kv.at[s],
            device_id=target(base + s, tp), device_id_type=pl.DeviceIdType.MESH,
        ).wait_recv()
        pltpu.make_async_remote_copy(
            src_ref=qs.at[s], dst_ref=qr.at[s],
            send_sem=s_q.at[s], recv_sem=r_q.at[s],
            device_id=target(base + s, tp), device_id_type=pl.DeviceIdType.MESH,
        ).wait_recv()
        ready(s)

    def attend(q, keys, b, o_old, t_old):
        s = lax.dot_general(q, keys, NT, preferred_element_type=F32) + b
        t_new = jnp.maximum(t_old, jnp.max(s, axis=1, keepdims=True))
        p = jnp.concatenate(
            [
                jnp.exp(s[:, c : c + BACK] - t_new).astype(BF16)
                for c in range(0, keys.shape[0], BACK)
            ],
            axis=1,
        )
        ones = jnp.where(iota(keys.shape, 1) < HD, jnp.ones_like(keys), keys)
        o = jnp.dot(p, ones, preferred_element_type=F32)
        return o_old * jnp.exp(t_old - t_new) + o, t_new

    def run(tiles):
        done = []
        for q, keys, b, where in tiles:
            shape = acc[where].shape
            o, t = attend(
                q, keys, b, acc[where].reshape(BACK, LANES), top[where].reshape(BACK, LANES)
            )
            done.append((where, o.reshape(shape), t.reshape(shape)))
        for where, o, t in done:
            acc[where] = o
            top[where] = t

    mine = slice(BACK, 2 * BACK)
    prior = slice(0, BACK)

    def tile1(h, part):
        keys = {None: pl.ds(own0 - 1 + h, 2), "own": own0 + h, "prior": own0 - 1 + h}[part]
        cols = {None: slice(None), "own": mine, "prior": prior}[part]
        return q2[h], kv[keys].reshape(-1, LANES), bias[0, :, cols], (h,)

    def tile4(quarter, r, part):
        rows = pl.ds(r * 32, 32)
        at = own0 + 4 * quarter
        keys = {None: slice(at - 4, at + 4), "own": slice(at, at + 4), "prior": slice(at - 4, at)}[part]
        cols = {None: slice(None), "own": mine, "prior": prior}[part]
        return (
            q2[4 * quarter : 4 * quarter + 4, rows, :].reshape(BACK, LANES),
            kv[keys, rows, :].reshape(-1, LANES),
            bias[1, :, cols],
            (slice(4 * quarter, 4 * quarter + 4), rows, slice(None)),
        )

    def tile16(r, part):
        rows = pl.ds(r * 8, 8)
        keys = {"own": slice(own0, 2 * own0), "prior": slice(0, own0)}[part]
        return (
            q2f[:, rows, :].reshape(BACK, LANES).astype(BF16),
            kvf[keys, rows, :].reshape(BACK, LANES).astype(BF16),
            bias[2, :, {"own": mine, "prior": prior}[part]],
            (slice(None), rows, slice(None)),
        )

    nq = G * halves

    @pl.loop(0, (nq - 1) // 3)
    def _(i):
        run([tile1(1 + 3 * i + n, None) for n in range(3)])

    run([tile1(0, "own")])

    @pl.loop(0, 4)
    def _(r):
        run([tile4(n, r, None) for n in range(1, nq // 4)])

    run([tile4(0, r, "own") for r in range(4)])

    @pl.loop(0, 4)
    def _(i):
        run([tile16(4 * i + n, "own") for n in range(4)])

    def arrive(s):
        pltpu.make_async_remote_copy(
            src_ref=kvs.at[s], dst_ref=kv.at[pl.ds(halves * s, halves)],
            send_sem=s_x.at[s], recv_sem=r_x.at[s],
            device_id=target(base - G + s, tp), device_id_type=pl.DeviceIdType.MESH,
        ).wait_recv()
        at = pl.ds(halves * s, halves)
        kvf[at] = kv[at].astype(F32)

    @pl.when(has_prev)
    def _():
        for s in range(G - 4 // halves, G):
            arrive(s)
        run([tile1(0, "prior")])
        run([tile4(0, r, "prior") for r in range(4)])
        for s in range(G - 4 // halves):
            arrive(s)

        @pl.loop(0, 4)
        def _(i):
            run([tile16(4 * i + n, "prior") for n in range(4)])

    @pl.loop(0, nq)
    def _(h):
        o = acc[h]
        y = o / pltpu.roll(o, HD, 1)
        rs[h] = jnp.where(low[: HD], pltpu.roll(y[:HD], HD, 1), y[HD:]).astype(BF16)

    def copy_ret(n):
        return pltpu.make_async_remote_copy(
            src_ref=rs.at[n], dst_ref=rr.at[head], send_sem=s_ret.at[n], recv_sem=r_ret.at[head],
            device_id=target(base + n // tp_count, lax.rem(n, tp_count)),
            device_id_type=pl.DeviceIdType.MESH,
        )

    for o in range(1, seats):
        copy_ret(lax.rem(seat + o, seats)).start()
    rr[head] = rs[seat]

    for o in range(1, G):
        copy_kv(lax.rem(me + o, G)).wait_send()
        copy_q(lax.rem(me + o, G)).wait_send()

    @pl.when(has_next)
    def _():
        for o in range(G):
            copy_x(lax.rem(me + o, G)).wait_send()

    w_local.wait()
    w_away.wait_send()
    pltpu.make_async_remote_copy(
        src_ref=w_ref, dst_ref=wbuf.at[tp_count - 1 - tp],
        send_sem=w_sem.at[1], recv_sem=w_sem.at[2],
        device_id=target(sp, tp_count - 1 - tp), device_id_type=pl.DeviceIdType.MESH,
    ).wait_recv()

    for o in range(1, seats):
        n = lax.rem(seat - o + seats, seats)
        their = lax.rem(n, tp_count) * G + n // tp_count
        pltpu.make_async_remote_copy(
            src_ref=rs.at[n], dst_ref=rr.at[their], send_sem=s_ret.at[n],
            recv_sem=r_ret.at[their],
            device_id=target(base + n // tp_count, lax.rem(n, tp_count)),
            device_id_type=pl.DeviceIdType.MESH,
        ).wait_recv()

    low_h = low[:HD]
    for m in range(seats // 2):
        x0 = rr[2 * m].astype(F32)
        x1 = rr[2 * m + 1].astype(F32)
        pair = jnp.concatenate(
            [jnp.where(low_h, x0, pltpu.roll(x1, HD, 1)), jnp.where(low_h, pltpu.roll(x0, HD, 1), x1)],
            axis=0,
        ).astype(BF16)
        mx[:, m * LANES : (m + 1) * LANES] = jnp.dot(
            back, pair, preferred_element_type=F32
        ).astype(BF16)

    width = wbuf.shape[1]
    step = 512

    @pl.loop(0, out_ref.shape[1] // step)
    def _(c):
        cols = pl.ds(pl.multiple_of(c * step, step), step)
        total = jnp.dot(mx[:, :width], wbuf[0, :, cols], preferred_element_type=F32)
        total = total + jnp.dot(mx[:, width:], wbuf[1, :, cols], preferred_element_type=F32)
        out_ref[:, cols] = total.astype(BF16)

    for o in range(1, seats):
        copy_ret(lax.rem(seat + o, seats)).wait_send()


def per_device(sp_count, tp_count, query_rows, key_rows, value_rows, out_weight):
    tok = query_rows.shape[0]
    G = query_rows.shape[1] // HD
    halves = tok // BACK
    ngroups = sp_count // G
    assert tok == 2 * BACK and tp_count == 2 and sp_count % G == 0
    assert G * tok == 16 * BACK
    inverse = np.power(THETA, -np.arange(HD // 2) / (HD // 2))
    inverse = np.tile(inverse, LANES // (HD // 2))[None, :]
    local = np.arange(tok)[:, None] * inverse
    cosb = jnp.asarray(np.cos(local), F32)
    sinb = jnp.asarray(np.sin(local), F32)
    inv = jnp.asarray(np.tile(inverse, (8, 1)), F32)
    seats = G * tp_count
    vmem = pl.BlockSpec(memory_space=pltpu.VMEM)
    dma = pltpu.SemaphoreType.DMA
    return pl.pallas_call(
        functools.partial(kernel, G, ngroups, tp_count),
        out_shape=jax.ShapeDtypeStruct((tok // tp_count, out_weight.shape[1]), BF16),
        in_specs=[pl.BlockSpec(memory_space=pl.ANY)] * 7,
        out_specs=vmem,
        scratch_shapes=[
            pltpu.VMEM(query_rows.shape, BF16),
            pltpu.VMEM(query_rows.shape, BF16),
            pltpu.VMEM(query_rows.shape, BF16),
            pltpu.VMEM(cosb.shape, F32),
            pltpu.VMEM(sinb.shape, F32),
            pltpu.VMEM(inv.shape, F32),
            pltpu.VMEM((G, BACK, LANES), BF16),
            pltpu.VMEM((G, halves, BACK, LANES), BF16),
            pltpu.VMEM((G, BACK, LANES), BF16),
            pltpu.VMEM((2 * G * halves, BACK, LANES), BF16),
            pltpu.VMEM((2 * G * halves, BACK, LANES), F32),
            pltpu.VMEM((G * halves, BACK, LANES), BF16),
            pltpu.VMEM((G * halves, BACK, LANES), F32),
            pltpu.VMEM((G * halves, BACK, LANES), F32),
            pltpu.VMEM((G * halves, BACK, LANES), F32),
            pltpu.VMEM((3, BACK, 2 * BACK), F32),
            pltpu.VMEM((tp_count,) + out_weight.shape, BF16),
            pltpu.VMEM((seats, HD, LANES), BF16),
            pltpu.VMEM((seats, HD, LANES), BF16),
            pltpu.VMEM((BACK, seats * HD), BF16),
            dma((G,)), dma((G,)), dma((G,)), dma((G,)), dma((G,)), dma((G,)),
            dma((3,)), dma((seats,)), dma((seats,)), dma((6,)),
        ],
        compiler_params=pltpu.CompilerParams(
            collective_id=0, has_side_effects=True, vmem_limit_bytes=63 * 1024 * 1024
        ),
    )(query_rows, key_rows, value_rows, cosb, sinb, inv, out_weight)


def solution(mesh):
    return jax.shard_map(
        functools.partial(per_device, mesh.shape["sp"], mesh.shape["tp"]),
        mesh=mesh,
        in_specs=(P("sp", "tp"), P("sp", "tp"), P("sp", "tp"), P("tp", None)),
        out_specs=P(("sp", "tp"), None),
        check_vma=False,
    )
```

```python
import functools
import math

import jax
import jax.numpy as jnp
import numpy as np
from jax import lax
from jax.experimental import pallas as pl
from jax.experimental.pallas import tpu as pltpu
from jax.sharding import PartitionSpec as P

HD = 64
BACK = 128
THETA = 500000.0
FAR = -1e30
F32 = jnp.float32
BF16 = jnp.bfloat16
LANES = 2 * HD
NT = (((1,), (1,)), ((), ()))


def place(p):
    return ((p & 7) << 4) + (((p >> 3) & 3) << 2) + (p >> 5)


def iota(shape, axis):
    return lax.broadcasted_iota(jnp.int32, shape, axis)


def kernel(
    G, ngroups, tp_count,
    q_hbm, k_hbm, v_hbm, cosb_hbm, sinb_hbm, inv_hbm, w_ref, out_ref,
    q_ref, k_ref, v_ref, cosb_ref, sinb_ref, inv_ref, qs, kvs, qr, kv, kvf, q2, q2f, acc, top, bias, wbuf, rs, rr, mx,
    s_kv, s_q, s_x, r_kv, r_q, r_x, w_sem, s_ret, r_ret, in_sem,
):
    loads = [
        pltpu.make_async_copy(source, dest, in_sem.at[n])
        for n, (source, dest) in enumerate((
            (inv_hbm, inv_ref), (cosb_hbm, cosb_ref), (sinb_hbm, sinb_ref),
            (k_hbm, k_ref), (v_hbm, v_ref), (q_hbm, q_ref),
        ))
    ]
    for load in loads:
        load.start()
    sp = lax.axis_index("sp")
    tp = lax.axis_index("tp")
    group = sp // G
    me = sp - group * G
    base = group * G
    has_prev = group > 0
    has_next = group < ngroups - 1
    seat = me * tp_count + tp
    seats = G * tp_count
    head = tp * G + me
    tok = q_ref.shape[0]
    halves = tok // BACK

    def target(s, t):
        return {"sp": s, "tp": t}

    barrier = pltpu.get_barrier_semaphore()
    for o in range(1, seats):
        n = lax.rem(seat + o, seats)
        pl.semaphore_signal(
            barrier, inc=1, device_id=target(base + n // tp_count, lax.rem(n, tp_count)),
            device_id_type=pl.DeviceIdType.MESH,
        )

    @pl.when(has_prev)
    def _():
        for o in range(G):
            pl.semaphore_signal(
                barrier, inc=1, device_id=target(base - G + o, tp),
                device_id_type=pl.DeviceIdType.MESH,
            )

    @pl.when(has_next)
    def _():
        for o in range(G):
            pl.semaphore_signal(
                barrier, inc=1, device_id=target(base + G + o, tp),
                device_id_type=pl.DeviceIdType.MESH,
            )

    w_local = pltpu.make_async_copy(w_ref, wbuf.at[tp], w_sem.at[0])
    w_local.start()

    for load in loads:
        load.wait()

    lane = iota((BACK, LANES), 1)
    low = lane < HD
    lane_t = iota((tok, LANES), 1)
    first = (lane_t & (HD - 1)) < HD // 2
    angle = inv_ref[...] * (sp * tok).astype(F32)
    ca = jnp.cos(angle)[:1]
    sa = jnp.sin(angle)[:1]
    cos = ca * cosb_ref[...] - sa * sinb_ref[...]
    sin = sa * cosb_ref[...] + ca * sinb_ref[...]
    sin = jnp.where(first, -sin, sin)
    swizzle = jnp.where(place(iota((BACK, BACK), 0)) == iota((BACK, BACK), 1), 1.0, 0.0).astype(BF16)
    back = jnp.where(place(iota((BACK, BACK), 1)) == iota((BACK, BACK), 0), 1.0, 0.0).astype(BF16)

    def turn(ref, cols):
        x = ref[:, cols].astype(F32)
        other = jnp.where(first, pltpu.roll(x, LANES - HD // 2, 1), pltpu.roll(x, HD // 2, 1))
        return (x * cos + other * sin).astype(BF16)

    def sw(x):
        return jnp.dot(swizzle, x, preferred_element_type=F32)

    for m in range(G // 2):
        cols = slice(m * LANES, (m + 1) * LANES)
        tq = turn(q_ref, cols)
        tk = turn(k_ref, cols)
        tv = v_ref[:, cols]
        qa = sw(tq[:BACK]) * (1.0 / math.sqrt(HD))
        qb = sw(tq[BACK:]) * (1.0 / math.sqrt(HD))
        qs[2 * m] = jnp.where(low, qa, pltpu.roll(qb, HD, 1)).astype(BF16)
        qs[2 * m + 1] = jnp.where(low, pltpu.roll(qa, HD, 1), qb).astype(BF16)
        for e in range(halves):
            ks = sw(tk[e * BACK : (e + 1) * BACK])
            vs = sw(tv[e * BACK : (e + 1) * BACK])
            kvs[2 * m, e] = jnp.where(low, ks, pltpu.roll(vs, HD, 1)).astype(BF16)
            kvs[2 * m + 1, e] = jnp.where(low, pltpu.roll(ks, HD, 1), vs).astype(BF16)

    pl.semaphore_wait(
        barrier, seats - 1 + jnp.where(has_prev, G, 0) + jnp.where(has_next, G, 0)
    )

    own0 = G * halves

    def copy_kv(dest):
        return pltpu.make_async_remote_copy(
            src_ref=kvs.at[dest], dst_ref=kv.at[pl.ds(own0 + halves * me, halves)],
            send_sem=s_kv.at[dest], recv_sem=r_kv.at[me],
            device_id=target(base + dest, tp), device_id_type=pl.DeviceIdType.MESH,
        )

    def copy_q(dest):
        return pltpu.make_async_remote_copy(
            src_ref=qs.at[dest], dst_ref=qr.at[me],
            send_sem=s_q.at[dest], recv_sem=r_q.at[me],
            device_id=target(base + dest, tp), device_id_type=pl.DeviceIdType.MESH,
        )

    def copy_x(dest):
        return pltpu.make_async_remote_copy(
            src_ref=kvs.at[dest], dst_ref=kv.at[pl.ds(halves * me, halves)],
            send_sem=s_x.at[dest], recv_sem=r_x.at[me],
            device_id=target(base + G + dest, tp), device_id_type=pl.DeviceIdType.MESH,
        )

    w_away = pltpu.make_async_remote_copy(
        src_ref=w_ref, dst_ref=wbuf.at[tp], send_sem=w_sem.at[1], recv_sem=w_sem.at[2],
        device_id=target(sp, tp_count - 1 - tp), device_id_type=pl.DeviceIdType.MESH,
    )

    bits = [1 << n for n in range(G.bit_length() - 1)]
    far = sorted(range(1, G), key=lambda o: -o.bit_count())

    def mate(o):
        return sum((((me // b + o // b) % 2) * b for b in bits), 0)

    for o in far:
        copy_kv(mate(o)).start()
        copy_q(mate(o)).start()

    @pl.when(has_next)
    def _():
        for o in range(G):
            copy_x(mate(o)).start()

    w_away.start()

    row = iota((BACK, 2 * BACK), 0)
    col = iota((BACK, 2 * BACK), 1)
    old = col < BACK
    missing = jnp.logical_and(old, group == 0)

    def stride4(n):
        w = n & 31
        return ((n >> 5) << 5) + ((w & 7) << 2) + (w >> 3)

    def masked(distance):
        return jnp.where((distance >= 0) & (distance <= BACK), 0.0, FAR)

    b1 = masked(place(row) + BACK - place(col & (BACK - 1)) - ((col >> 7) << 7))
    b4 = masked(stride4(row) + BACK - stride4(col))
    b16 = masked(row + BACK - col)
    bias[0] = b1
    bias[1] = b4
    bias[2] = jnp.where(missing, FAR, b1)
    bias[3] = jnp.where(missing, FAR, b4)
    bias[4] = jnp.where(missing, FAR, b16)

    acc[...] = jnp.zeros_like(acc)
    top[...] = jnp.full_like(top, FAR)

    @pl.when(jnp.logical_not(has_prev))
    def _():
        kv[:own0] = jnp.zeros((own0, BACK, LANES), BF16)

    kv[pl.ds(own0 + halves * me, halves)] = kvs[me]
    qr[me] = qs[me]

    def ready(s):
        x = qr[s].astype(F32)
        a = jnp.where(low, x, 0.0)
        b = jnp.where(low, pltpu.roll(x, HD, 1), 0.0)
        q2f[2 * s] = a
        q2f[2 * s + 1] = b
        q2[2 * s] = a.astype(BF16)
        q2[2 * s + 1] = b.astype(BF16)
        at = pl.ds(own0 + halves * s, halves)
        kvf[at] = kv[at].astype(F32)

    ready(me)
    for o in range(1, G):
        s = lax.rem(me - o + G, G)
        pltpu.make_async_remote_copy(
            src_ref=kvs.at[s], dst_ref=kv.at[pl.ds(own0 + halves * s, halves)],
            send_sem=s_kv.at[s], recv_sem=r_kv.at[s],
            device_id=target(base + s, tp), device_id_type=pl.DeviceIdType.MESH,
        ).wait_recv()
        pltpu.make_async_remote_copy(
            src_ref=qs.at[s], dst_ref=qr.at[s],
            send_sem=s_q.at[s], recv_sem=r_q.at[s],
            device_id=target(base + s, tp), device_id_type=pl.DeviceIdType.MESH,
        ).wait_recv()
        ready(s)

    low_keys = iota((2 * BACK, LANES), 1) < HD

    def attend(q, keys, b, o_old, t_old):
        s = lax.dot_general(q, keys, NT, preferred_element_type=F32) + b
        t_new = jnp.maximum(t_old, jnp.max(s, axis=1, keepdims=True))
        p = jnp.concatenate(
            [jnp.exp(s[:, :BACK] - t_new), jnp.exp(s[:, BACK:] - t_new)], axis=1
        ).astype(BF16)
        ones = jnp.where(low_keys, jnp.ones_like(keys), keys)
        o = jnp.dot(p, ones, preferred_element_type=F32)
        return o_old * jnp.exp(t_old - t_new) + o, t_new

    def run(tiles):
        done = []
        for q, keys, b, where in tiles:
            shape = acc[where].shape
            o, t = attend(
                q, keys, b, acc[where].reshape(BACK, LANES), top[where].reshape(BACK, LANES)
            )
            done.append((where, o.reshape(shape), t.reshape(shape)))
        for where, o, t in done:
            acc[where] = o
            top[where] = t

    def tile1(h, b):
        return (
            q2[h], kv[pl.ds(own0 - 1 + h, 2)].reshape(2 * BACK, LANES), bias[b], (h,),
        )

    def tile4(quarter, r, b):
        rows = pl.ds(r * 32, 32)
        return (
            q2[4 * quarter : 4 * quarter + 4, rows, :].reshape(BACK, LANES),
            kv[own0 + 4 * quarter - 4 : own0 + 4 * quarter + 4, rows, :].reshape(2 * BACK, LANES),
            bias[b],
            (slice(4 * quarter, 4 * quarter + 4), rows, slice(None)),
        )

    def tile16(r):
        rows = pl.ds(r * 8, 8)
        return (
            q2f[:, rows, :].reshape(BACK, LANES).astype(BF16),
            kvf[:, rows, :].reshape(2 * BACK, LANES).astype(BF16),
            bias[4],
            (slice(None), rows, slice(None)),
        )

    nq = G * halves

    @pl.loop(0, (nq - 1) // 3)
    def _(i):
        run([tile1(1 + 3 * i + n, 0) for n in range(3)])

    @pl.loop(0, 4)
    def _(r):
        run([tile4(n, r, 1) for n in range(1, nq // 4)])

    @pl.when(has_prev)
    def _():
        for o in range(G):
            s = lax.rem(me - o + G, G)
            pltpu.make_async_remote_copy(
                src_ref=kvs.at[s], dst_ref=kv.at[pl.ds(halves * s, halves)],
                send_sem=s_x.at[s], recv_sem=r_x.at[s],
                device_id=target(base - G + s, tp), device_id_type=pl.DeviceIdType.MESH,
            ).wait_recv()

    @pl.loop(0, G)
    def _(i):
        at = pl.ds(2 * i, 2)
        kvf[at] = kv[at].astype(F32)

    run([tile1(0, 2)])
    run([tile4(0, r, 3) for r in range(4)])

    @pl.loop(0, 4)
    def _(i):
        run([tile16(4 * i + n) for n in range(4)])

    @pl.loop(0, nq)
    def _(h):
        o = acc[h]
        y = o / pltpu.roll(o, HD, 1)
        rs[h] = jnp.where(low[: HD], pltpu.roll(y[:HD], HD, 1), y[HD:]).astype(BF16)

    def copy_ret(n):
        return pltpu.make_async_remote_copy(
            src_ref=rs.at[n], dst_ref=rr.at[head], send_sem=s_ret.at[n], recv_sem=r_ret.at[head],
            device_id=target(base + n // tp_count, lax.rem(n, tp_count)),
            device_id_type=pl.DeviceIdType.MESH,
        )

    for o in far + [0]:
        copy_ret(mate(o) * tp_count + tp_count - 1 - tp).start()
        if o:
            copy_ret(mate(o) * tp_count + tp).start()
    rr[head] = rs[seat]

    for o in range(1, G):
        copy_kv(lax.rem(me + o, G)).wait_send()
        copy_q(lax.rem(me + o, G)).wait_send()

    @pl.when(has_next)
    def _():
        for o in range(G):
            copy_x(lax.rem(me + o, G)).wait_send()

    w_local.wait()
    w_away.wait_send()
    pltpu.make_async_remote_copy(
        src_ref=w_ref, dst_ref=wbuf.at[tp_count - 1 - tp],
        send_sem=w_sem.at[1], recv_sem=w_sem.at[2],
        device_id=target(sp, tp_count - 1 - tp), device_id_type=pl.DeviceIdType.MESH,
    ).wait_recv()

    for o in range(1, seats):
        n = lax.rem(seat - o + seats, seats)
        their = lax.rem(n, tp_count) * G + n // tp_count
        pltpu.make_async_remote_copy(
            src_ref=rs.at[n], dst_ref=rr.at[their], send_sem=s_ret.at[n],
            recv_sem=r_ret.at[their],
            device_id=target(base + n // tp_count, lax.rem(n, tp_count)),
            device_id_type=pl.DeviceIdType.MESH,
        ).wait_recv()

    low_h = low[:HD]
    for m in range(seats // 2):
        x0 = rr[2 * m].astype(F32)
        x1 = rr[2 * m + 1].astype(F32)
        pair = jnp.concatenate(
            [jnp.where(low_h, x0, pltpu.roll(x1, HD, 1)), jnp.where(low_h, pltpu.roll(x0, HD, 1), x1)],
            axis=0,
        ).astype(BF16)
        mx[:, m * LANES : (m + 1) * LANES] = jnp.dot(
            back, pair, preferred_element_type=F32
        ).astype(BF16)

    width = wbuf.shape[1]
    step = 512

    @pl.loop(0, out_ref.shape[1] // step)
    def _(c):
        cols = pl.ds(pl.multiple_of(c * step, step), step)
        total = jnp.dot(mx[:, :width], wbuf[0, :, cols], preferred_element_type=F32)
        total = total + jnp.dot(mx[:, width:], wbuf[1, :, cols], preferred_element_type=F32)
        out_ref[:, cols] = total.astype(BF16)

    for o in range(1, seats):
        copy_ret(lax.rem(seat + o, seats)).wait_send()


def per_device(sp_count, tp_count, query_rows, key_rows, value_rows, out_weight):
    tok = query_rows.shape[0]
    G = query_rows.shape[1] // HD
    halves = tok // BACK
    ngroups = sp_count // G
    assert tok == 2 * BACK and tp_count == 2 and sp_count % G == 0
    assert G & (G - 1) == 0
    assert G * tok == 16 * BACK
    inverse = np.power(THETA, -np.arange(HD // 2) / (HD // 2))
    inverse = np.tile(inverse, LANES // (HD // 2))[None, :]
    local = np.arange(tok)[:, None] * inverse
    cosb = jnp.asarray(np.cos(local), F32)
    sinb = jnp.asarray(np.sin(local), F32)
    inv = jnp.asarray(np.tile(inverse, (8, 1)), F32)
    seats = G * tp_count
    vmem = pl.BlockSpec(memory_space=pltpu.VMEM)
    dma = pltpu.SemaphoreType.DMA
    return pl.pallas_call(
        functools.partial(kernel, G, ngroups, tp_count),
        out_shape=jax.ShapeDtypeStruct((tok // tp_count, out_weight.shape[1]), BF16),
        in_specs=[pl.BlockSpec(memory_space=pl.ANY)] * 7,
        out_specs=vmem,
        scratch_shapes=[
            pltpu.VMEM(query_rows.shape, BF16),
            pltpu.VMEM(query_rows.shape, BF16),
            pltpu.VMEM(query_rows.shape, BF16),
            pltpu.VMEM(cosb.shape, F32),
            pltpu.VMEM(sinb.shape, F32),
            pltpu.VMEM(inv.shape, F32),
            pltpu.VMEM((G, BACK, LANES), BF16),
            pltpu.VMEM((G, halves, BACK, LANES), BF16),
            pltpu.VMEM((G, BACK, LANES), BF16),
            pltpu.VMEM((2 * G * halves, BACK, LANES), BF16),
            pltpu.VMEM((2 * G * halves, BACK, LANES), F32),
            pltpu.VMEM((G * halves, BACK, LANES), BF16),
            pltpu.VMEM((G * halves, BACK, LANES), F32),
            pltpu.VMEM((G * halves, BACK, LANES), F32),
            pltpu.VMEM((G * halves, BACK, LANES), F32),
            pltpu.VMEM((5, BACK, 2 * BACK), F32),
            pltpu.VMEM((tp_count,) + out_weight.shape, BF16),
            pltpu.VMEM((seats, HD, LANES), BF16),
            pltpu.VMEM((seats, HD, LANES), BF16),
            pltpu.VMEM((BACK, seats * HD), BF16),
            dma((G,)), dma((G,)), dma((G,)), dma((G,)), dma((G,)), dma((G,)),
            dma((3,)), dma((seats,)), dma((seats,)), dma((6,)),
        ],
        compiler_params=pltpu.CompilerParams(
            collective_id=0, has_side_effects=True, vmem_limit_bytes=63 * 1024 * 1024
        ),
    )(query_rows, key_rows, value_rows, cosb, sinb, inv, out_weight)


def solution(mesh):
    return jax.shard_map(
        functools.partial(per_device, mesh.shape["sp"], mesh.shape["tp"]),
        mesh=mesh,
        in_specs=(P("sp", "tp"), P("sp", "tp"), P("sp", "tp"), P("tp", None)),
        out_specs=P(("sp", "tp"), None),
        check_vma=False,
    )
```

```python
import functools
import math

import jax
import jax.numpy as jnp
import numpy as np
from jax import lax
from jax.experimental import pallas as pl
from jax.experimental.pallas import tpu as pltpu
from jax.sharding import PartitionSpec as P

HD = 64
BACK = 128
THETA = 500000.0
FAR = -1e30
F32 = jnp.float32
BF16 = jnp.bfloat16
LANES = 2 * HD
NT = (((1,), (1,)), ((), ()))


def place(p):
    return ((p & 7) << 4) + (((p >> 3) & 3) << 2) + (p >> 5)


def iota(shape, axis):
    return lax.broadcasted_iota(jnp.int32, shape, axis)


def kernel(
    G, ngroups, tp_count,
    q_hbm, k_hbm, v_hbm, cosb_hbm, sinb_hbm, inv_hbm, w_ref, out_ref,
    q_ref, k_ref, v_ref, cosb_ref, sinb_ref, inv_ref, qs, kvs, qr, kv, kvf, q2, q2f, acc, top, bias, wbuf, rs, rr, mx,
    s_kv, s_q, s_x, r_kv, r_q, r_x, w_sem, s_ret, r_ret, in_sem,
):
    loads = [
        pltpu.make_async_copy(source, dest, in_sem.at[n])
        for n, (source, dest) in enumerate((
            (inv_hbm, inv_ref), (cosb_hbm, cosb_ref), (sinb_hbm, sinb_ref),
            (k_hbm, k_ref), (v_hbm, v_ref), (q_hbm, q_ref),
        ))
    ]
    for load in loads:
        load.start()
    sp = lax.axis_index("sp")
    tp = lax.axis_index("tp")
    group = sp // G
    me = sp - group * G
    base = group * G
    has_prev = group > 0
    has_next = group < ngroups - 1
    seat = me * tp_count + tp
    seats = G * tp_count
    head = tp * G + me
    tok = q_ref.shape[0]
    halves = tok // BACK

    def target(s, t):
        return {"sp": s, "tp": t}

    barrier = pltpu.get_barrier_semaphore()
    for o in range(1, seats):
        n = lax.rem(seat + o, seats)
        pl.semaphore_signal(
            barrier, inc=1, device_id=target(base + n // tp_count, lax.rem(n, tp_count)),
            device_id_type=pl.DeviceIdType.MESH,
        )

    @pl.when(has_prev)
    def _():
        for o in range(G):
            pl.semaphore_signal(
                barrier, inc=1, device_id=target(base - G + o, tp),
                device_id_type=pl.DeviceIdType.MESH,
            )

    @pl.when(has_next)
    def _():
        for o in range(G):
            pl.semaphore_signal(
                barrier, inc=1, device_id=target(base + G + o, tp),
                device_id_type=pl.DeviceIdType.MESH,
            )

    w_local = pltpu.make_async_copy(w_ref, wbuf.at[tp], w_sem.at[0])
    w_local.start()

    for load in loads:
        load.wait()

    lane = iota((BACK, LANES), 1)
    low = lane < HD
    lane_t = iota((tok, LANES), 1)
    first = (lane_t & (HD - 1)) < HD // 2
    angle = inv_ref[...] * (sp * tok).astype(F32)
    ca = jnp.cos(angle)[:1]
    sa = jnp.sin(angle)[:1]
    cos = ca * cosb_ref[...] - sa * sinb_ref[...]
    sin = sa * cosb_ref[...] + ca * sinb_ref[...]
    sin = jnp.where(first, -sin, sin)
    swizzle = jnp.where(place(iota((BACK, BACK), 0)) == iota((BACK, BACK), 1), 1.0, 0.0).astype(BF16)
    back = jnp.where(place(iota((BACK, BACK), 1)) == iota((BACK, BACK), 0), 1.0, 0.0).astype(BF16)

    def turn(ref, cols):
        x = ref[:, cols].astype(F32)
        other = jnp.where(first, pltpu.roll(x, LANES - HD // 2, 1), pltpu.roll(x, HD // 2, 1))
        return (x * cos + other * sin).astype(BF16)

    def sw(x):
        return jnp.dot(swizzle, x, preferred_element_type=F32)

    for m in range(G // 2):
        cols = slice(m * LANES, (m + 1) * LANES)
        tq = turn(q_ref, cols)
        tk = turn(k_ref, cols)
        tv = v_ref[:, cols]
        qa = sw(tq[:BACK]) * (1.0 / math.sqrt(HD))
        qb = sw(tq[BACK:]) * (1.0 / math.sqrt(HD))
        qs[2 * m] = jnp.where(low, qa, pltpu.roll(qb, HD, 1)).astype(BF16)
        qs[2 * m + 1] = jnp.where(low, pltpu.roll(qa, HD, 1), qb).astype(BF16)
        for e in range(halves):
            ks = sw(tk[e * BACK : (e + 1) * BACK])
            vs = sw(tv[e * BACK : (e + 1) * BACK])
            kvs[2 * m, e] = jnp.where(low, ks, pltpu.roll(vs, HD, 1)).astype(BF16)
            kvs[2 * m + 1, e] = jnp.where(low, pltpu.roll(ks, HD, 1), vs).astype(BF16)

    pl.semaphore_wait(
        barrier, seats - 1 + jnp.where(has_prev, G, 0) + jnp.where(has_next, G, 0)
    )

    own0 = G * halves

    def copy_kv(dest):
        return pltpu.make_async_remote_copy(
            src_ref=kvs.at[dest], dst_ref=kv.at[pl.ds(own0 + halves * me, halves)],
            send_sem=s_kv.at[dest], recv_sem=r_kv.at[me],
            device_id=target(base + dest, tp), device_id_type=pl.DeviceIdType.MESH,
        )

    def copy_q(dest):
        return pltpu.make_async_remote_copy(
            src_ref=qs.at[dest], dst_ref=qr.at[me],
            send_sem=s_q.at[dest], recv_sem=r_q.at[me],
            device_id=target(base + dest, tp), device_id_type=pl.DeviceIdType.MESH,
        )

    def copy_x(dest):
        return pltpu.make_async_remote_copy(
            src_ref=kvs.at[dest], dst_ref=kv.at[pl.ds(halves * me, halves)],
            send_sem=s_x.at[dest], recv_sem=r_x.at[me],
            device_id=target(base + G + dest, tp), device_id_type=pl.DeviceIdType.MESH,
        )

    w_away = pltpu.make_async_remote_copy(
        src_ref=w_ref, dst_ref=wbuf.at[tp], send_sem=w_sem.at[1], recv_sem=w_sem.at[2],
        device_id=target(sp, tp_count - 1 - tp), device_id_type=pl.DeviceIdType.MESH,
    )

    bits = [1 << n for n in range(G.bit_length() - 1)]
    far = sorted(range(1, G), key=lambda o: -o.bit_count())

    def mate(o):
        return sum((((me // b + o // b) % 2) * b for b in bits), 0)

    for o in far:
        copy_kv(mate(o)).start()
        copy_q(mate(o)).start()

    @pl.when(has_next)
    def _():
        for o in range(G):
            copy_x(mate(o)).start()

    w_away.start()

    row = iota((BACK, 2 * BACK), 0)
    col = iota((BACK, 2 * BACK), 1)
    old = col < BACK
    missing = jnp.logical_and(old, group == 0)

    def stride4(n):
        w = n & 31
        return ((n >> 5) << 5) + ((w & 7) << 2) + (w >> 3)

    def masked(distance):
        return jnp.where((distance >= 0) & (distance <= BACK), 0.0, FAR)

    b1 = masked(place(row) + BACK - place(col & (BACK - 1)) - ((col >> 7) << 7))
    b4 = masked(stride4(row) + BACK - stride4(col))
    b16 = masked(row + BACK - col)
    bias[0] = b1
    bias[1] = b4
    bias[2] = jnp.where(missing, FAR, b1)
    bias[3] = jnp.where(missing, FAR, b4)
    bias[4] = jnp.where(missing, FAR, b16)

    acc[...] = jnp.zeros_like(acc)
    top[...] = jnp.full_like(top, FAR)

    @pl.when(jnp.logical_not(has_prev))
    def _():
        kv[:own0] = jnp.zeros((own0, BACK, LANES), BF16)

    kv[pl.ds(own0 + halves * me, halves)] = kvs[me]
    qr[me] = qs[me]

    def ready(s):
        x = qr[s].astype(F32)
        a = jnp.where(low, x, 0.0)
        b = jnp.where(low, pltpu.roll(x, HD, 1), 0.0)
        q2f[2 * s] = a
        q2f[2 * s + 1] = b
        q2[2 * s] = a.astype(BF16)
        q2[2 * s + 1] = b.astype(BF16)
        at = pl.ds(own0 + halves * s, halves)
        kvf[at] = kv[at].astype(F32)

    ready(me)
    for o in range(1, G):
        s = lax.rem(me - o + G, G)
        pltpu.make_async_remote_copy(
            src_ref=kvs.at[s], dst_ref=kv.at[pl.ds(own0 + halves * s, halves)],
            send_sem=s_kv.at[s], recv_sem=r_kv.at[s],
            device_id=target(base + s, tp), device_id_type=pl.DeviceIdType.MESH,
        ).wait_recv()
        pltpu.make_async_remote_copy(
            src_ref=qs.at[s], dst_ref=qr.at[s],
            send_sem=s_q.at[s], recv_sem=r_q.at[s],
            device_id=target(base + s, tp), device_id_type=pl.DeviceIdType.MESH,
        ).wait_recv()
        ready(s)

    low_keys = iota((2 * BACK, LANES), 1) < HD

    def attend(q, keys, b, o_old, t_old):
        s = lax.dot_general(q, keys, NT, preferred_element_type=F32) + b
        t_new = jnp.maximum(t_old, jnp.max(s, axis=1, keepdims=True))
        p = jnp.concatenate(
            [jnp.exp(s[:, :BACK] - t_new), jnp.exp(s[:, BACK:] - t_new)], axis=1
        ).astype(BF16)
        ones = jnp.where(low_keys, jnp.ones_like(keys), keys)
        o = jnp.dot(p, ones, preferred_element_type=F32)
        return o_old * jnp.exp(t_old - t_new) + o, t_new

    def run(tiles):
        done = []
        for q, keys, b, where in tiles:
            shape = acc[where].shape
            o, t = attend(
                q, keys, b, acc[where].reshape(BACK, LANES), top[where].reshape(BACK, LANES)
            )
            done.append((where, o.reshape(shape), t.reshape(shape)))
        for where, o, t in done:
            acc[where] = o
            top[where] = t

    def tile1(h, b):
        return (
            q2[h], kv[pl.ds(own0 - 1 + h, 2)].reshape(2 * BACK, LANES), bias[b], (h,),
        )

    def tile4(quarter, r, b):
        rows = pl.ds(r * 32, 32)
        return (
            q2[4 * quarter : 4 * quarter + 4, rows, :].reshape(BACK, LANES),
            kv[own0 + 4 * quarter - 4 : own0 + 4 * quarter + 4, rows, :].reshape(2 * BACK, LANES),
            bias[b],
            (slice(4 * quarter, 4 * quarter + 4), rows, slice(None)),
        )

    def tile16(r):
        rows = pl.ds(r * 8, 8)
        return (
            q2f[:, rows, :].reshape(BACK, LANES).astype(BF16),
            kvf[:, rows, :].reshape(2 * BACK, LANES).astype(BF16),
            bias[4],
            (slice(None), rows, slice(None)),
        )

    nq = G * halves

    @pl.loop(0, (nq - 1) // 3)
    def _(i):
        run([tile1(1 + 3 * i + n, 0) for n in range(3)])

    @pl.loop(0, 4)
    def _(r):
        run([tile4(n, r, 1) for n in range(1, nq // 4)])

    def arrive(sources):
        @pl.when(has_prev)
        def _():
            for s in sources:
                at = pl.ds(halves * s, halves)
                pltpu.make_async_remote_copy(
                    src_ref=kvs.at[s], dst_ref=kv.at[at], send_sem=s_x.at[s], recv_sem=r_x.at[s],
                    device_id=target(base - G + s, tp), device_id_type=pl.DeviceIdType.MESH,
                ).wait_recv()
                kvf[at] = kv[at].astype(F32)

    @pl.when(jnp.logical_not(has_prev))
    def _():
        kvf[:own0] = jnp.zeros((own0, BACK, LANES), F32)

    arrive(range(G - 4 // halves, G))
    run([tile1(0, 2)])
    run([tile4(0, r, 3) for r in range(4)])

    arrive(range(G - 4 // halves))

    @pl.loop(0, 4)
    def _(i):
        run([tile16(4 * i + n) for n in range(4)])

    @pl.loop(0, nq)
    def _(h):
        o = acc[h]
        y = o / pltpu.roll(o, HD, 1)
        rs[h] = jnp.where(low[: HD], pltpu.roll(y[:HD], HD, 1), y[HD:]).astype(BF16)

    def copy_ret(n):
        return pltpu.make_async_remote_copy(
            src_ref=rs.at[n], dst_ref=rr.at[head], send_sem=s_ret.at[n], recv_sem=r_ret.at[head],
            device_id=target(base + n // tp_count, lax.rem(n, tp_count)),
            device_id_type=pl.DeviceIdType.MESH,
        )

    for o in far + [0]:
        copy_ret(mate(o) * tp_count + tp_count - 1 - tp).start()
        if o:
            copy_ret(mate(o) * tp_count + tp).start()
    rr[head] = rs[seat]

    for o in range(1, G):
        copy_kv(lax.rem(me + o, G)).wait_send()
        copy_q(lax.rem(me + o, G)).wait_send()

    @pl.when(has_next)
    def _():
        for o in range(G):
            copy_x(lax.rem(me + o, G)).wait_send()

    w_local.wait()
    w_away.wait_send()
    pltpu.make_async_remote_copy(
        src_ref=w_ref, dst_ref=wbuf.at[tp_count - 1 - tp],
        send_sem=w_sem.at[1], recv_sem=w_sem.at[2],
        device_id=target(sp, tp_count - 1 - tp), device_id_type=pl.DeviceIdType.MESH,
    ).wait_recv()

    for o in range(1, seats):
        n = lax.rem(seat - o + seats, seats)
        their = lax.rem(n, tp_count) * G + n // tp_count
        pltpu.make_async_remote_copy(
            src_ref=rs.at[n], dst_ref=rr.at[their], send_sem=s_ret.at[n],
            recv_sem=r_ret.at[their],
            device_id=target(base + n // tp_count, lax.rem(n, tp_count)),
            device_id_type=pl.DeviceIdType.MESH,
        ).wait_recv()

    low_h = low[:HD]
    for m in range(seats // 2):
        x0 = rr[2 * m].astype(F32)
        x1 = rr[2 * m + 1].astype(F32)
        pair = jnp.concatenate(
            [jnp.where(low_h, x0, pltpu.roll(x1, HD, 1)), jnp.where(low_h, pltpu.roll(x0, HD, 1), x1)],
            axis=0,
        ).astype(BF16)
        mx[:, m * LANES : (m + 1) * LANES] = jnp.dot(
            back, pair, preferred_element_type=F32
        ).astype(BF16)

    width = wbuf.shape[1]
    step = 512

    @pl.loop(0, out_ref.shape[1] // step)
    def _(c):
        cols = pl.ds(pl.multiple_of(c * step, step), step)
        total = jnp.dot(mx[:, :width], wbuf[0, :, cols], preferred_element_type=F32)
        total = total + jnp.dot(mx[:, width:], wbuf[1, :, cols], preferred_element_type=F32)
        out_ref[:, cols] = total.astype(BF16)

    for o in range(1, seats):
        copy_ret(lax.rem(seat + o, seats)).wait_send()


def per_device(sp_count, tp_count, query_rows, key_rows, value_rows, out_weight):
    tok = query_rows.shape[0]
    G = query_rows.shape[1] // HD
    halves = tok // BACK
    ngroups = sp_count // G
    assert tok == 2 * BACK and tp_count == 2 and sp_count % G == 0
    assert G & (G - 1) == 0
    assert G * tok == 16 * BACK
    inverse = np.power(THETA, -np.arange(HD // 2) / (HD // 2))
    inverse = np.tile(inverse, LANES // (HD // 2))[None, :]
    local = np.arange(tok)[:, None] * inverse
    cosb = jnp.asarray(np.cos(local), F32)
    sinb = jnp.asarray(np.sin(local), F32)
    inv = jnp.asarray(np.tile(inverse, (8, 1)), F32)
    seats = G * tp_count
    vmem = pl.BlockSpec(memory_space=pltpu.VMEM)
    dma = pltpu.SemaphoreType.DMA
    return pl.pallas_call(
        functools.partial(kernel, G, ngroups, tp_count),
        out_shape=jax.ShapeDtypeStruct((tok // tp_count, out_weight.shape[1]), BF16),
        in_specs=[pl.BlockSpec(memory_space=pl.ANY)] * 7,
        out_specs=vmem,
        scratch_shapes=[
            pltpu.VMEM(query_rows.shape, BF16),
            pltpu.VMEM(query_rows.shape, BF16),
            pltpu.VMEM(query_rows.shape, BF16),
            pltpu.VMEM(cosb.shape, F32),
            pltpu.VMEM(sinb.shape, F32),
            pltpu.VMEM(inv.shape, F32),
            pltpu.VMEM((G, BACK, LANES), BF16),
            pltpu.VMEM((G, halves, BACK, LANES), BF16),
            pltpu.VMEM((G, BACK, LANES), BF16),
            pltpu.VMEM((2 * G * halves, BACK, LANES), BF16),
            pltpu.VMEM((2 * G * halves, BACK, LANES), F32),
            pltpu.VMEM((G * halves, BACK, LANES), BF16),
            pltpu.VMEM((G * halves, BACK, LANES), F32),
            pltpu.VMEM((G * halves, BACK, LANES), F32),
            pltpu.VMEM((G * halves, BACK, LANES), F32),
            pltpu.VMEM((5, BACK, 2 * BACK), F32),
            pltpu.VMEM((tp_count,) + out_weight.shape, BF16),
            pltpu.VMEM((seats, HD, LANES), BF16),
            pltpu.VMEM((seats, HD, LANES), BF16),
            pltpu.VMEM((BACK, seats * HD), BF16),
            dma((G,)), dma((G,)), dma((G,)), dma((G,)), dma((G,)), dma((G,)),
            dma((3,)), dma((seats,)), dma((seats,)), dma((6,)),
        ],
        compiler_params=pltpu.CompilerParams(
            collective_id=0, has_side_effects=True, vmem_limit_bytes=63 * 1024 * 1024
        ),
    )(query_rows, key_rows, value_rows, cosb, sinb, inv, out_weight)


def solution(mesh):
    return jax.shard_map(
        functools.partial(per_device, mesh.shape["sp"], mesh.shape["tp"]),
        mesh=mesh,
        in_specs=(P("sp", "tp"), P("sp", "tp"), P("sp", "tp"), P("tp", None)),
        out_specs=P(("sp", "tp"), None),
        check_vma=False,
    )
```
